32 devices in a mesh: ep: 8 (over z, x), tp: 4 (over y, core).
Axes of the slice: x: 2, y: 2, z: 4, core: 2. Of those that a mesh axis runs over, the one named last changes fastest.
Arguments:
- tokens: bfloat16 [1024, 2048], P('ep', 'tp'), may hold values from -36 to 36
- cotangent: bfloat16 [1024, 2048], P('ep', 'tp'), may hold values from -6 to 6
- routes: int32 [1024, 2], P('ep'), may hold values from 0 to 7, all different within a row; in each aligned block of 128 rows (0 to 127, 128 to 255, ...) at most 33 rows name the same one
- route_weights: bfloat16 [1024, 2], P('ep'), may hold values from 0.099609375 to 1
- gate_weight: bfloat16 [8, 2048, 1024], P('ep', None, 'tp'), may hold values from -0.125 to 0.125
- up_weight: bfloat16 [8, 2048, 1024], P('ep', None, 'tp'), may hold values from -0.125 to 0.125
- down_weight: bfloat16 [8, 1024, 2048], P('ep', 'tp'), may hold values from -0.1875 to 0.1875
Outputs:
- token_grad: bfloat16 [1024, 2048], P('ep', 'tp')
- weight_grad: bfloat16 [1024, 2], P('ep')
- down_grad: bfloat16 [8, 1024, 2048], P('ep', 'tp')
The draws below stay inside these ranges and needn't reach their ends.
Inputs may be any that keep to these rules, and one draw needn't show every extreme that they name: `routes`: each row names 2 different experts; within the rows of one device of ep (aligned blocks of 128 rows) no expert is named more than 33 times.
All inputs are finite; a program needn't handle non-finite values.
Results may differ from the reference program's by a relative error of at most 0.013.
Values may be sent and summed in bfloat16 or wider, within the bound.
No kernel may reach another device: no remote copies, remote signals or barrier semaphores. Data moves between devices by JAX's collectives and lax.ppermute only.
A program may use at most 64 MiB of HBM per device.

```python
import math
import jax
import jax.numpy as jnp
import numpy as np
from jax import lax

D = 2048
F = 1024
TOPK = 2
TOK_DEV = 128
EXPERTS = 8
CAP = 33
TOKENS = 1024
N_EP = 8
N_TP = 4


def draw_tokens(key, part):
    values = jax.random.truncated_normal(key, -6.0, 6.0, (TOKENS, D), jnp.float32)
    return values.astype(jnp.bfloat16)


def block_scale(key, shape, split, least, high):
    factor_of, own = 1.0, jax.random.fold_in(key, 6)
    for position, shards_of in split:
        draws = jnp.exp(jax.random.uniform(jax.random.fold_in(own, position), (shards_of,), jnp.float32, least / len(split), high / len(split)))
        factor_of = factor_of * jnp.repeat(draws, shape[position] // shards_of).reshape([-1 if axis == position else 1 for axis in range(len(shape))])
    return factor_of


def routed_block(rng, own, number, rows, amount, top, bound, lean):
    ranking = jax.random.permutation(rng, amount)
    crowded, common = portions_of(amount, rows * top, bound, lean, True), portions_of(amount, rows * top, bound, lean, False)
    places = jnp.arange(amount)

    def named(sizes, offset_by):
        used = int((sizes > 0).sum())
        fixed = max(1, used // 4)
        moved = fixed + (places - fixed + offset_by * (used - fixed)) % max(1, amount - fixed)
        return jnp.zeros((amount,), jnp.int32).at[ranking[jnp.where(places < fixed, places, moved)]].set(jnp.asarray(sizes, jnp.int32))

    sizes = jnp.where(number % 4 == 0, named(crowded, number // 4), named(common, number - number // 4 - 1))
    mixed = jax.random.permutation(jax.random.fold_in(own, 3), amount)
    giver, receiver = mixed[0:amount // 2 * 2:2], mixed[1:amount // 2 * 2:2]
    margin = jnp.minimum(sizes[giver] - 1, bound - sizes[receiver]) // 2
    margin = jnp.where((giver == ranking[0]) | (receiver == ranking[0]) | (sizes[receiver] == 0), 0, jnp.maximum(margin, 0))
    moved = jax.random.randint(jax.random.fold_in(own, 4), (amount // 2,), 0, 1 << 20) % (margin + 1)
    sizes = sizes.at[giver].add(-moved).at[receiver].add(moved)
    labels = jnp.searchsorted(jnp.cumsum(sizes), jnp.arange(rows * top), side="right").astype(jnp.int32)
    grid = labels.reshape(top, rows).T
    grid = grid[jax.random.permutation(jax.random.fold_in(own, 1), rows)]
    offset_by = jax.random.randint(jax.random.fold_in(own, 2), (rows, 1), 0, top)
    return jnp.take_along_axis(grid, (jnp.arange(top)[None, :] + offset_by) % top, axis=1)


def portions_of(number_of, total, most, skew, full):
    weights = [(1 << 20) // math.isqrt(rank ** skew) + 1 for rank in range(1, number_of + 1)]
    largest = most if full else min(most, max(-(-total // number_of), total * weights[0] // sum(weights)))
    least = 1 if total - largest >= number_of - 1 else 0
    counts, rest = [largest] + [least] * (number_of - 1), total - largest - least * (number_of - 1)
    while rest > 0:
        movable = [i for i in range(1, number_of) if counts[i] < largest] or [i for i in range(1, number_of) if counts[i] < most]
        pool, budget = sum([weights[i] for i in movable]), rest
        for i in movable:
            extra = min(most - counts[i], max(1, budget * weights[i] // pool), rest)
            counts[i] = counts[i] + extra
            rest = rest - extra
    return np.array(counts)


def noise(rng, extent, scale, bound, pieces=(), kind=jnp.bfloat16):
    values = jax.random.normal(rng, extent, jnp.float32) * scale
    if len(pieces) > 0:
        values = block_scale(rng, extent, pieces, -0.22, 0.18) * values
    return jnp.clip(values, min=-bound, max=bound).astype(kind)


def setup_inputs(seed: int = 0) -> dict:
    seeds = jax.random.split(jax.random.key(seed), 8)
    tokens = draw_tokens(jax.random.fold_in(seeds[7], 71), 0)
    cotangent = noise(seeds[1], (TOKENS, D), 1.0, 6.0, ((0, 8), (1, 4)))
    routes_keys = jax.random.split(jax.random.fold_in(seeds[2], 1), TOKENS // TOK_DEV)
    routes_turns = jax.random.permutation(jax.random.fold_in(seeds[2], 3), TOKENS // TOK_DEV)
    routes = jax.vmap(lambda own, number: routed_block(jax.random.fold_in(seeds[2], 2), own, number, TOK_DEV, EXPERTS, TOPK, CAP, 2))(routes_keys, routes_turns).reshape((TOKENS, TOPK))
    route_weights = jnp.clip(0.099609375 + 0.9003906 * jax.random.uniform(seeds[3], (TOKENS, TOPK), jnp.float32) ** block_scale(seeds[3], (TOKENS, TOPK), ((0, 8),), -0.2, 0.2), 0.099609375, 1.0).astype(jnp.bfloat16)
    gate_weight = noise(seeds[4], (EXPERTS, D, F), D ** -0.5, 0.125, ((0, 8), (2, 4)))
    up_weight = noise(seeds[5], (EXPERTS, D, F), D ** -0.5, 0.125, ((0, 8), (2, 4)))
    down_weight = noise(seeds[6], (EXPERTS, F, D), F ** -0.5, 0.1875, ((0, 8), (1, 4)))
    return {"tokens": tokens, "cotangent": cotangent, "routes": routes, "route_weights": route_weights, "gate_weight": gate_weight, "up_weight": up_weight, "down_weight": down_weight}


clamp_limit = 7.0
alpha_gate = 1.702


def ranks_within(route_block, experts):
    flat_routes = route_block.reshape(-1)
    onehot = (flat_routes[:, None] == jnp.arange(experts, dtype=jnp.int32)[None, :]).astype(jnp.int32)
    before = jnp.cumsum(onehot, axis=0) - onehot
    return jnp.sum(before * onehot, axis=1).astype(jnp.int32)


def expert_terms(exp_rows, exp_grads, scales, gate_mat, up_mat, down_mat):
    gate_pre = jnp.dot(exp_rows, gate_mat, preferred_element_type=jnp.float32)
    up_pre = jnp.dot(exp_rows, up_mat, preferred_element_type=jnp.float32)
    gate_clip = jnp.minimum(gate_pre, clamp_limit)
    up_clip = jnp.clip(up_pre, -clamp_limit, clamp_limit)
    sigmoid_gate = jax.nn.sigmoid(alpha_gate * gate_clip)
    swish_gate = gate_clip * sigmoid_gate
    hidden = (up_clip + 1.0) * swish_gate
    back_proj = lax.dot_general(exp_grads, down_mat, (((1,), (1,)), ((), ())), preferred_element_type=jnp.float32)
    scores = jnp.sum(hidden * back_proj, axis=1)
    weight_col = scales.astype(jnp.float32)[:, None]
    scaled = back_proj * weight_col
    slope = sigmoid_gate + alpha_gate * swish_gate * (1.0 - sigmoid_gate)
    gate_grad = jnp.where(gate_pre < clamp_limit, scaled * (up_clip + 1.0) * slope, 0.0).astype(jnp.bfloat16)
    up_grad = jnp.where(jnp.abs(up_pre) < clamp_limit, scaled * swish_gate, 0.0).astype(jnp.bfloat16)
    weighted = (hidden * weight_col).astype(jnp.bfloat16)
    down_part = lax.dot_general(weighted, exp_grads, (((0,), (0,)), ((), ())), preferred_element_type=jnp.float32)
    token_part = lax.dot_general(gate_grad, gate_mat, (((1,), (1,)), ((), ())), preferred_element_type=jnp.float32)
    token_part = token_part + lax.dot_general(up_grad, up_mat, (((1,), (1,)), ((), ())), preferred_element_type=jnp.float32)
    return token_part, scores, down_part


def reference(tokens, cotangent, routes, route_weights, gate_weight, up_weight, down_weight):
    experts = gate_weight.shape[0]
    slot_count = N_EP * CAP
    blocks = routes.reshape(N_EP, TOK_DEV, TOPK)
    slot_ranks = jax.vmap(lambda block: ranks_within(block, experts))(blocks).reshape(-1)
    flat_routes = routes.reshape(-1)
    source = jnp.arange(TOKENS * TOPK, dtype=jnp.int32) // (TOK_DEV * TOPK)
    slot_place = (flat_routes * slot_count + source * CAP + slot_ranks).astype(jnp.int32)
    slot_owner = jnp.full((experts * slot_count,), -1, jnp.int32)
    slot_owner = slot_owner.at[slot_place].set(jnp.arange(TOKENS * TOPK, dtype=jnp.int32)).reshape(experts, slot_count)
    flat_weights = route_weights.reshape(-1)
    width_block = F // N_TP

    def one_expert(inputs):
        slot_table, gate_mat, up_mat, down_mat = inputs
        filled = slot_table >= 0
        pair_index = jnp.where(filled, slot_table, 0)
        token_index = pair_index // TOPK
        exp_rows = jnp.where(filled[:, None], tokens[token_index], 0).astype(jnp.bfloat16)
        exp_grads = jnp.where(filled[:, None], cotangent[token_index], 0).astype(jnp.bfloat16)
        scales = jnp.where(filled, flat_weights[pair_index], 0).astype(jnp.bfloat16)
        token_total = jnp.zeros((slot_count, D), jnp.float32)
        score_total = jnp.zeros((slot_count,), jnp.float32)
        down_parts = []
        for part_index in range(N_TP):
            low = part_index * width_block
            token_part, scores, down_part = expert_terms(
                exp_rows, exp_grads, scales, gate_mat[:, low:low + width_block],
                up_mat[:, low:low + width_block], down_mat[low:low + width_block, :])
            token_total = token_total + token_part.astype(jnp.bfloat16).astype(jnp.float32)
            score_total = score_total + scores
            down_parts.append(down_part)
        down_full = jnp.concatenate(down_parts, axis=0)
        return token_total.astype(jnp.bfloat16), score_total, down_full.astype(jnp.bfloat16)

    token_parts, score_parts, down_grad = lax.map(one_expert, (slot_owner, gate_weight, up_weight, down_weight))
    gathered = token_parts.reshape(experts * slot_count, D)[slot_place].reshape(TOKENS, TOPK, D)
    token_grad = jnp.sum(gathered.astype(jnp.float32), axis=1).astype(jnp.bfloat16)
    weight_grad = score_parts.reshape(-1)[slot_place].reshape(TOKENS, TOPK).astype(jnp.bfloat16)
    return token_grad, weight_grad, down_grad
```

```python
import functools
import jax
import jax.numpy as jnp
from jax import lax
from jax.experimental import pallas as pl
from jax.experimental.pallas import tpu as pltpu
from jax.sharding import PartitionSpec as P

clamp_limit = 7.0
alpha_gate = 1.702
lanes = 128


VMEM = pl.BlockSpec(memory_space=pltpu.VMEM)
SMEM = pl.BlockSpec(memory_space=pltpu.SMEM)
f32 = jnp.float32
bf16 = jnp.bfloat16


def iota(shape, dim):
    return lax.broadcasted_iota(jnp.int32, shape, dim)


def to_row(col):
    diag = iota((col.shape[0], lanes), 0) == iota((col.shape[0], lanes), 1)
    return jnp.sum(jnp.where(diag, col, 0.0), axis=0, keepdims=True)


def to_col(row, rows):
    diag = iota((rows, lanes), 0) == iota((rows, lanes), 1)
    return jnp.sum(jnp.where(diag, row, 0.0), axis=1, keepdims=True)


def call(body, out, name, flops=0, nbytes=0):
    def run(scalars, *args):
        return pl.pallas_call(
            body,
            out_shape=out,
            in_specs=[SMEM] + [VMEM] * len(args),
            out_specs=jax.tree.map(lambda _: VMEM, out),
            name=name,
            cost_estimate=pl.CostEstimate(
                flops=flops, bytes_accessed=nbytes, transcendentals=0
            ),
        )(scalars, *args)

    return run


def places(me, routes_t, experts):
    top, rows = routes_t.shape
    ids = iota((experts, rows), 0)
    named = [ids == (routes_t[k : k + 1, :] ^ me) for k in range(top)]
    any_named = functools.reduce(jnp.logical_or, named)
    before = (iota((rows, rows), 0) < iota((rows, rows), 1)).astype(bf16)
    ranks = jnp.dot(any_named.astype(bf16), before, preferred_element_type=f32)
    return named, jnp.where(any_named, ranks, -1.0)


def picks(pos, pad):
    experts, rows = pos.shape
    want = iota((pad, rows), 0).astype(f32)
    return jnp.concatenate(
        [(pos[e : e + 1, :] == want).astype(bf16) for e in range(experts)], axis=0
    )


def dispatch_body(cap, pad, split, s_ref, routes_ref, weights_ref, tok_ref, cot_ref, *outs):
    routes_t = routes_ref[...]
    top, rows = routes_t.shape
    depth = tok_ref.shape[1]
    experts = outs[0].shape[0] if not split else len(outs)
    named, pos = places(s_ref[0], routes_t, experts)
    weights = weights_ref[...].astype(f32)
    scale = functools.reduce(
        jnp.add, [jnp.where(named[k], weights[k : k + 1, :], 0.0) for k in range(top)]
    )
    pick = picks(pos, pad)
    rows_x = jnp.dot(pick, tok_ref[...], preferred_element_type=f32).astype(bf16)
    rows_g = jnp.dot(pick, cot_ref[...], preferred_element_type=f32).astype(bf16)
    extra = iota((pad, lanes), 0) == cap
    for e in range(experts):
        out = outs[e] if split else outs[0].at[e]
        low, high = e * pad, (e + 1) * pad
        col = jnp.sum(
            pick[low:high, :].astype(f32) * scale[e : e + 1, :], axis=1, keepdims=True
        )
        head = jnp.where(extra, to_row(col), rows_x[low:high, :lanes].astype(f32))
        out[:, :lanes] = head.astype(bf16)
        out[:, lanes:depth] = rows_x[low:high, lanes:]
        out[:, depth:] = rows_g[low:high, :]


def expert_body(cap, pad, s_ref, gate_ref, up_ref, down_ref, *refs):
    n_parts = (len(refs) - 3)
    parts, (send_ref, keep_ref, weighted_ref) = refs[:n_parts], refs[n_parts:]
    total, wide = parts[0].shape
    depth = wide // 2
    blocks = total // pad

    def feats(j):
        return pl.ds(pl.multiple_of(s_ref[j] * depth, lanes), depth)

    gate_pre = up_pre = back = None
    for j in range(n_parts):
        x, g = parts[j][:, :depth], parts[j][:, depth:]
        a = jnp.dot(x, gate_ref[feats(j), :], preferred_element_type=f32)
        b = jnp.dot(x, up_ref[feats(j), :], preferred_element_type=f32)
        c = lax.dot_general(
            g, down_ref[:, feats(j)], (((1,), (1,)), ((), ())), preferred_element_type=f32
        )
        gate_pre = a if gate_pre is None else gate_pre + a
        up_pre = b if up_pre is None else up_pre + b
        back = c if back is None else back + c
    gate_clip = jnp.minimum(gate_pre, clamp_limit)
    up_one = jnp.clip(up_pre, -clamp_limit, clamp_limit) + 1.0
    sig = jax.nn.sigmoid(alpha_gate * gate_clip)
    swish = gate_clip * sig
    hidden = up_one * swish
    scores = jnp.sum(hidden * back, axis=1, keepdims=True)
    weight = jnp.concatenate(
        [
            to_col(parts[0][b * pad + cap : b * pad + cap + 1, :lanes].astype(f32), pad)
            for b in range(blocks)
        ],
        axis=0,
    )
    scaled = back * weight
    slope = sig + alpha_gate * swish * (1.0 - sig)
    gate_grad = jnp.where(gate_pre < clamp_limit, scaled * up_one * slope, 0.0).astype(bf16)
    up_grad = jnp.where(jnp.abs(up_pre) < clamp_limit, scaled * swish, 0.0).astype(bf16)
    weighted_ref[...] = (hidden * weight).astype(bf16)
    for j in range(n_parts):
        part = lax.dot_general(
            gate_grad, gate_ref[feats(j), :], (((1,), (1,)), ((), ())), preferred_element_type=f32
        ) + lax.dot_general(
            up_grad, up_ref[feats(j), :], (((1,), (1,)), ((), ())), preferred_element_type=f32
        )
        out = send_ref if j % 2 else keep_ref
        out[:, (j // 2) * depth : (j // 2 + 1) * depth] = part.astype(bf16)
    row_of = iota((pad, lanes), 0)
    for b in range(blocks):
        low, high = b * pad, (b + 1) * pad
        row = to_row(scores[low:high, :])
        first = row.astype(bf16).astype(f32)
        for out in (send_ref, keep_ref):
            for half in range(n_parts // 2):
                at = slice(half * depth, half * depth + lanes)
                tile = out[low:high, at].astype(f32)
                tile = jnp.where(row_of == cap, first, tile)
                tile = jnp.where(row_of == cap + 1, row - first, tile)
                out[low:high, at] = tile.astype(bf16)


def resplit(cap, pad, tile):
    row_of = iota((pad, lanes), 0)
    pieces = []
    for b in range(tile.shape[0] // pad):
        t = tile[b * pad : (b + 1) * pad, :]
        row = t[cap : cap + 1, :] + t[cap + 1 : cap + 2, :]
        first = row.astype(bf16).astype(f32)
        t = jnp.where(row_of == cap, first, t)
        pieces.append(jnp.where(row_of == cap + 1, row - first, t))
    return jnp.concatenate(pieces, axis=0)


def add_body(cap, pad, s_ref, a_ref, b_ref, *outs):
    wide = a_ref.shape[1]
    tot = a_ref[...].astype(f32) + b_ref[...].astype(f32)
    depth = wide // 2
    keep_ref, send_ref = outs
    keep_ref[...] = tot[:, :depth]
    send_ref[:, lanes:] = tot[:, depth + lanes :].astype(bf16)
    send_ref[:, :lanes] = resplit(cap, pad, tot[:, depth : depth + lanes]).astype(bf16)


def last_body(cap, pad, s_ref, a_ref, b_ref, *outs):
    tot = a_ref[...] + b_ref[...].astype(f32)
    head = resplit(cap, pad, tot[:, :lanes]).astype(bf16)
    if len(outs) == 1:
        outs[0][:, :lanes] = head
        outs[0][:, lanes:] = tot[:, lanes:].astype(bf16)
        return
    for b, out in enumerate(outs):
        out[:, :lanes] = head[b * pad : (b + 1) * pad, :]
        out[:, lanes:] = tot[b * pad : (b + 1) * pad, lanes:].astype(bf16)


def down_body(n_parts, s_ref, *refs):
    out = refs[-1]
    groups = refs[:-1]
    depth = groups[1].shape[1] // 2
    for j in range(n_parts):
        acc = None
        for g in range(0, len(groups), n_parts + 1):
            part = lax.dot_general(
                groups[g][...],
                groups[g + 1 + j][:, depth:],
                (((0,), (0,)), ((), ())),
                preferred_element_type=f32,
            )
            acc = part if acc is None else acc + part
        at = pl.ds(pl.multiple_of(s_ref[j] * depth, lanes), depth)
        out[:, at] = acc.astype(bf16)


def combine_body(cap, pad, experts, s_ref, routes_ref, *refs):
    blocks, (tok_ref, wgt_ref) = refs[:-2], refs[-2:]
    routes_t = routes_ref[...]
    top = routes_t.shape[0]
    named, pos = places(s_ref[0], routes_t, experts)
    pick = picks(pos, pad)
    if len(blocks) == 1:
        rows = blocks[0][...]
    else:
        rows = jnp.concatenate([b[...] for b in blocks], axis=0)
    tok_ref[...] = lax.dot_general(
        pick, rows, (((0,), (0,)), ((), ())), preferred_element_type=f32
    ).astype(bf16)
    scores = []
    for e in range(experts):
        low = e * pad
        row = rows[low + cap : low + cap + 1, :lanes].astype(f32)
        row = row + rows[low + cap + 1 : low + cap + 2, :lanes].astype(f32)
        col = to_col(row, pad)
        scores.append(
            jnp.sum(pick[low : low + pad, :].astype(f32) * col, axis=0, keepdims=True)
        )
    scores = jnp.concatenate(scores, axis=0)
    for k in range(top):
        wgt_ref[k : k + 1, :] = jnp.sum(
            jnp.where(named[k], scores, 0.0), axis=0, keepdims=True
        ).astype(bf16)


def struct(shape, dtype=bf16):
    return jax.ShapeDtypeStruct(shape, dtype)


def per_device(tokens, cotangent, routes, route_weights, gate_weight, up_weight, down_weight):
    experts = lax.axis_size("ep")
    shares = lax.axis_size("tp")
    rows, top = routes.shape
    depth = tokens.shape[1]
    width = gate_weight.shape[2]
    cap = rows * top // experts + 1
    pad = -(-(cap + 2) // 8) * 8
    by_permute = experts <= 8
    me = lax.axis_index("ep")
    mine = lax.axis_index("tp")
    rel = (me if by_permute else jnp.zeros_like(me)).astype(jnp.int32).reshape(1)
    order = jnp.stack([mine ^ j for j in range(shares)]).astype(jnp.int32)
    gate, up, down = gate_weight[0], up_weight[0], down_weight[0]
    routes_t, weights_t = routes.T, route_weights.T

    def over_tp(v, flip):
        return lax.ppermute(v, "tp", [(i, i ^ flip) for i in range(shares)])

    def over_ep(v, flip):
        return lax.ppermute(v, "ep", [(i, i ^ flip) for i in range(experts)])

    if by_permute:
        out = [struct((pad, 2 * depth))] * experts
    else:
        out = [struct((experts, pad, 2 * depth))]
    blocks = call(
        functools.partial(dispatch_body, cap, pad, by_permute), out, "dispatch",
        flops=4 * experts * pad * rows * depth,
    )(rel, routes_t, weights_t, tokens, cotangent)
    if by_permute:
        half = experts // 2
        moved = [blocks[0]] + [over_ep(blocks[k], k) for k in range(1, experts)]
        groups = [
            jnp.concatenate(moved[low : low + half], axis=0) for low in (0, half)
        ]
    else:
        got = lax.all_to_all(blocks[0], "ep", split_axis=0, concat_axis=0, tiled=True)
        groups = [got.reshape(experts * pad, 2 * depth)]
    n_rows = groups[0].shape[0]

    down_args, returned = [], []
    for own in groups:
        across = over_tp(own, 2)
        parts = [own, over_tp(own, 1), across, over_tp(across, 1)]
        send, keep, weighted = call(
            functools.partial(expert_body, cap, pad),
            [struct((n_rows, 2 * depth))] * 2 + [struct((n_rows, width))],
            "expert",
            flops=10 * n_rows * shares * depth * width,
        )(order, gate, up, down, *parts)
        down_args += [weighted] + parts
        got = over_tp(send, 1)
        keep, send = call(
            functools.partial(add_body, cap, pad),
            [struct((n_rows, depth), f32), struct((n_rows, depth))],
            "add",
            flops=n_rows * depth,
        )(rel, keep, got)
        got = over_tp(send, 2)
        if by_permute:
            out = [struct((pad, depth))] * (n_rows // pad)
        else:
            out = [struct((n_rows, depth))]
        returned += call(
            functools.partial(last_body, cap, pad), out, "last", flops=n_rows * depth
        )(rel, keep, got)
    if by_permute:
        returned = [returned[0]] + [over_ep(returned[k], k) for k in range(1, experts)]
    else:
        back = lax.all_to_all(
            returned[0].reshape(experts, pad, depth), "ep", split_axis=0, concat_axis=0, tiled=True
        )
        returned = [back.reshape(experts * pad, depth)]
    down_grad = call(
        functools.partial(down_body, shares),
        struct((width, shares * depth)),
        "down",
        flops=2 * experts * pad * width * shares * depth,
    )(order, *down_args)
    token_grad, weight_grad = call(
        functools.partial(combine_body, cap, pad, experts),
        [struct((rows, depth)), struct((top, rows))],
        "combine",
        flops=2 * experts * pad * rows * depth,
    )(rel, routes_t, *returned)
    return (token_grad, weight_grad.T, down_grad[None])


def solution(mesh):
    placed = (
        P("ep", "tp"),
        P("ep", "tp"),
        P("ep", None),
        P("ep", None),
        P("ep", None, "tp"),
        P("ep", None, "tp"),
        P("ep", "tp", None),
    )
    return jax.shard_map(
        per_device,
        mesh=mesh,
        in_specs=placed,
        out_specs=(P("ep", "tp"), P("ep", None), P("ep", "tp", None)),
        check_vma=False,
    )
```

```python
import functools
import jax
import jax.numpy as jnp
from jax import lax
from jax.experimental import pallas as pl
from jax.experimental.pallas import tpu as pltpu
from jax.sharding import PartitionSpec as P

clamp_limit = 7.0
alpha_gate = 1.702
lanes = 128


VMEM = pl.BlockSpec(memory_space=pltpu.VMEM)
SMEM = pl.BlockSpec(memory_space=pltpu.SMEM)
f32 = jnp.float32
bf16 = jnp.bfloat16


def iota(shape, dim):
    return lax.broadcasted_iota(jnp.int32, shape, dim)


def to_row(col):
    diag = iota((col.shape[0], lanes), 0) == iota((col.shape[0], lanes), 1)
    return jnp.sum(jnp.where(diag, col, 0.0), axis=0, keepdims=True)


def to_col(row, rows):
    diag = iota((rows, lanes), 0) == iota((rows, lanes), 1)
    return jnp.sum(jnp.where(diag, row, 0.0), axis=1, keepdims=True)


def call(body, out, name, flops=0, nbytes=0):
    def run(scalars, *args):
        return pl.pallas_call(
            body,
            out_shape=out,
            in_specs=[SMEM] + [VMEM] * len(args),
            out_specs=jax.tree.map(lambda _: VMEM, out),
            name=name,
            compiler_params=pltpu.CompilerParams(vmem_limit_bytes=24 << 20),
            cost_estimate=pl.CostEstimate(
                flops=flops, bytes_accessed=nbytes, transcendentals=0
            ),
        )(scalars, *args)

    return run


def places(me, routes_t, experts):
    top, rows = routes_t.shape
    ids = iota((experts, rows), 0)
    named = [ids == (routes_t[k : k + 1, :] ^ me) for k in range(top)]
    any_named = functools.reduce(jnp.logical_or, named)
    before = (iota((rows, rows), 0) < iota((rows, rows), 1)).astype(bf16)
    ranks = jnp.dot(any_named.astype(bf16), before, preferred_element_type=f32)
    return named, jnp.where(any_named, ranks, -1.0)


def picks(pos, pad):
    experts, rows = pos.shape
    want = iota((pad, rows), 0).astype(f32)
    return jnp.concatenate(
        [(pos[e : e + 1, :] == want).astype(bf16) for e in range(experts)], axis=0
    )


def dispatch_body(cap, pad, split, s_ref, routes_ref, weights_ref, tok_ref, cot_ref, *outs):
    routes_t = routes_ref[...]
    top, rows = routes_t.shape
    depth = tok_ref.shape[1]
    experts = outs[0].shape[0] if not split else len(outs)
    named, pos = places(s_ref[0], routes_t, experts)
    weights = weights_ref[...].astype(f32)
    scale = functools.reduce(
        jnp.add, [jnp.where(named[k], weights[k : k + 1, :], 0.0) for k in range(top)]
    )
    pick = picks(pos, pad)
    rows_x = jnp.dot(pick, tok_ref[...], preferred_element_type=f32).astype(bf16)
    rows_g = jnp.dot(pick, cot_ref[...], preferred_element_type=f32).astype(bf16)
    extra = iota((pad, lanes), 0) == cap
    for e in range(experts):
        out = outs[e] if split else outs[0].at[e]
        low, high = e * pad, (e + 1) * pad
        col = jnp.sum(
            pick[low:high, :].astype(f32) * scale[e : e + 1, :], axis=1, keepdims=True
        )
        head = jnp.where(extra, to_row(col), rows_x[low:high, :lanes].astype(f32))
        out[:, :lanes] = head.astype(bf16)
        out[:, lanes:depth] = rows_x[low:high, lanes:]
        out[:, depth:] = rows_g[low:high, :]


def expert_body(cap, pad, s_ref, gate_ref, up_ref, down_ref, *refs):
    n_parts = (len(refs) - 3)
    parts, (send_ref, keep_ref, weighted_ref) = refs[:n_parts], refs[n_parts:]
    total, wide = parts[0].shape
    depth = wide // 2
    blocks = total // pad

    def feats(j):
        return pl.ds(pl.multiple_of((s_ref[0] ^ j) * depth, lanes), depth)

    gate_pre = up_pre = back = None
    for j in range(n_parts):
        x, g = parts[j][:, :depth], parts[j][:, depth:]
        a = jnp.dot(x, gate_ref[feats(j), :], preferred_element_type=f32)
        b = jnp.dot(x, up_ref[feats(j), :], preferred_element_type=f32)
        c = lax.dot_general(
            g, down_ref[:, feats(j)], (((1,), (1,)), ((), ())), preferred_element_type=f32
        )
        gate_pre = a if gate_pre is None else gate_pre + a
        up_pre = b if up_pre is None else up_pre + b
        back = c if back is None else back + c
    gate_clip = jnp.minimum(gate_pre, clamp_limit)
    up_one = jnp.clip(up_pre, -clamp_limit, clamp_limit) + 1.0
    sig = jax.nn.sigmoid(alpha_gate * gate_clip)
    swish = gate_clip * sig
    hidden = up_one * swish
    scores = jnp.sum(hidden * back, axis=1, keepdims=True)
    weight = jnp.concatenate(
        [
            to_col(parts[0][b * pad + cap : b * pad + cap + 1, :lanes].astype(f32), pad)
            for b in range(blocks)
        ],
        axis=0,
    )
    scaled = back * weight
    slope = sig + alpha_gate * swish * (1.0 - sig)
    gate_grad = jnp.where(gate_pre < clamp_limit, scaled * up_one * slope, 0.0).astype(bf16)
    up_grad = jnp.where(jnp.abs(up_pre) < clamp_limit, scaled * swish, 0.0).astype(bf16)
    weighted_ref[...] = (hidden * weight).astype(bf16)
    for j in range(n_parts):
        part = lax.dot_general(
            gate_grad, gate_ref[feats(j), :], (((1,), (1,)), ((), ())), preferred_element_type=f32
        ) + lax.dot_general(
            up_grad, up_ref[feats(j), :], (((1,), (1,)), ((), ())), preferred_element_type=f32
        )
        out = send_ref if j % 2 else keep_ref
        out[:, (j // 2) * depth : (j // 2 + 1) * depth] = part.astype(bf16)
    row_of = iota((pad, lanes), 0)
    for b in range(blocks):
        low, high = b * pad, (b + 1) * pad
        row = to_row(scores[low:high, :])
        first = row.astype(bf16).astype(f32)
        for out in (send_ref, keep_ref):
            for half in range(n_parts // 2):
                at = slice(half * depth, half * depth + lanes)
                tile = out[low:high, at].astype(f32)
                tile = jnp.where(row_of == cap, first, tile)
                tile = jnp.where(row_of == cap + 1, row - first, tile)
                out[low:high, at] = tile.astype(bf16)


def resplit(cap, pad, tile):
    row_of = iota((pad, lanes), 0)
    pieces = []
    for b in range(tile.shape[0] // pad):
        t = tile[b * pad : (b + 1) * pad, :]
        row = t[cap : cap + 1, :] + t[cap + 1 : cap + 2, :]
        first = row.astype(bf16).astype(f32)
        t = jnp.where(row_of == cap, first, t)
        pieces.append(jnp.where(row_of == cap + 1, row - first, t))
    return jnp.concatenate(pieces, axis=0)


def add_body(cap, pad, s_ref, a_ref, b_ref, *outs):
    wide = a_ref.shape[1]
    tot = a_ref[...].astype(f32) + b_ref[...].astype(f32)
    depth = wide // 2
    keep_ref, send_ref = outs
    keep_ref[...] = tot[:, :depth]
    send_ref[:, lanes:] = tot[:, depth + lanes :].astype(bf16)
    send_ref[:, :lanes] = resplit(cap, pad, tot[:, depth : depth + lanes]).astype(bf16)


def last_body(cap, pad, s_ref, a_ref, b_ref, *outs):
    tot = a_ref[...] + b_ref[...].astype(f32)
    head = resplit(cap, pad, tot[:, :lanes]).astype(bf16)
    if len(outs) == 1:
        outs[0][:, :lanes] = head
        outs[0][:, lanes:] = tot[:, lanes:].astype(bf16)
        return
    for b, out in enumerate(outs):
        out[:, :lanes] = head[b * pad : (b + 1) * pad, :]
        out[:, lanes:] = tot[b * pad : (b + 1) * pad, lanes:].astype(bf16)


def down_body(n_parts, s_ref, *refs):
    out = refs[-1]
    groups = refs[:-1]
    depth = groups[1].shape[1] // 2
    for j in range(n_parts):
        acc = None
        for g in range(0, len(groups), n_parts + 1):
            part = lax.dot_general(
                groups[g][...],
                groups[g + 1 + j][:, depth:],
                (((0,), (0,)), ((), ())),
                preferred_element_type=f32,
            )
            acc = part if acc is None else acc + part
        at = pl.ds(pl.multiple_of((s_ref[0] ^ j) * depth, lanes), depth)
        out[:, at] = acc.astype(bf16)


def combine_body(cap, pad, experts, s_ref, routes_ref, *refs):
    blocks, (tok_ref, wgt_ref) = refs[:-2], refs[-2:]
    routes_t = routes_ref[...]
    top = routes_t.shape[0]
    named, pos = places(s_ref[0], routes_t, experts)
    pick = picks(pos, pad)
    if len(blocks) == 1:
        rows = blocks[0][...]
    else:
        rows = jnp.concatenate([b[...] for b in blocks], axis=0)
    tok_ref[...] = lax.dot_general(
        pick, rows, (((0,), (0,)), ((), ())), preferred_element_type=f32
    ).astype(bf16)
    scores = []
    for e in range(experts):
        low = e * pad
        row = rows[low + cap : low + cap + 1, :lanes].astype(f32)
        row = row + rows[low + cap + 1 : low + cap + 2, :lanes].astype(f32)
        col = to_col(row, pad)
        scores.append(
            jnp.sum(pick[low : low + pad, :].astype(f32) * col, axis=0, keepdims=True)
        )
    scores = jnp.concatenate(scores, axis=0)
    for k in range(top):
        wgt_ref[k : k + 1, :] = jnp.sum(
            jnp.where(named[k], scores, 0.0), axis=0, keepdims=True
        ).astype(bf16)


def struct(shape, dtype=bf16):
    return jax.ShapeDtypeStruct(shape, dtype)


def per_device(tokens, cotangent, routes, route_weights, gate_weight, up_weight, down_weight):
    experts = lax.axis_size("ep")
    shares = lax.axis_size("tp")
    rows, top = routes.shape
    depth = tokens.shape[1]
    width = gate_weight.shape[2]
    cap = rows * top // experts + 1
    pad = -(-(cap + 2) // 8) * 8
    by_permute = experts <= 8
    me = lax.axis_index("ep")
    mine = lax.axis_index("tp")
    rel = (me if by_permute else jnp.zeros_like(me)).astype(jnp.int32).reshape(1)
    share = mine.astype(jnp.int32).reshape(1)
    gate, up, down = gate_weight[0], up_weight[0], down_weight[0]
    routes_t, weights_t = routes.T, route_weights.T

    def over_tp(v, flip):
        return lax.ppermute(v, "tp", [(i, i ^ flip) for i in range(shares)])

    def over_ep(v, flip):
        return lax.ppermute(v, "ep", [(i, i ^ flip) for i in range(experts)])

    if by_permute:
        out = [struct((pad, 2 * depth))] * experts
    else:
        out = [struct((experts, pad, 2 * depth))]
    blocks = call(
        functools.partial(dispatch_body, cap, pad, by_permute), out, "dispatch",
        flops=4 * experts * pad * rows * depth,
    )(rel, routes_t, weights_t, tokens, cotangent)
    if by_permute:
        half = experts // 2
        moved = [blocks[0]] + [over_ep(blocks[k], k) for k in range(1, experts)]
        groups = [
            jnp.concatenate(moved[low : low + half], axis=0) for low in (0, half)
        ]
    else:
        got = lax.all_to_all(blocks[0], "ep", split_axis=0, concat_axis=0, tiled=True)
        groups = [got.reshape(experts * pad, 2 * depth)]
    n_rows = groups[0].shape[0]

    down_args, returned = [], []
    for own in groups:
        across = over_tp(own, 2)
        parts = [own, over_tp(own, 1), across, over_tp(across, 1)]
        send, keep, weighted = call(
            functools.partial(expert_body, cap, pad),
            [struct((n_rows, 2 * depth))] * 2 + [struct((n_rows, width))],
            "expert",
            flops=10 * n_rows * shares * depth * width,
        )(share, gate, up, down, *parts)
        down_args += [weighted] + parts
        got = over_tp(send, 1)
        keep, send = call(
            functools.partial(add_body, cap, pad),
            [struct((n_rows, depth), f32), struct((n_rows, depth))],
            "add",
            flops=n_rows * depth,
        )(rel, keep, got)
        got = over_tp(send, 2)
        if by_permute:
            out = [struct((pad, depth))] * (n_rows // pad)
        else:
            out = [struct((n_rows, depth))]
        returned += call(
            functools.partial(last_body, cap, pad), out, "last", flops=n_rows * depth
        )(rel, keep, got)
    if by_permute:
        returned = [returned[0]] + [over_ep(returned[k], k) for k in range(1, experts)]
    else:
        back = lax.all_to_all(
            returned[0].reshape(experts, pad, depth), "ep", split_axis=0, concat_axis=0, tiled=True
        )
        returned = [back.reshape(experts * pad, depth)]
    down_grad = call(
        functools.partial(down_body, shares),
        struct((width, shares * depth)),
        "down",
        flops=2 * experts * pad * width * shares * depth,
    )(share, *down_args)
    token_grad, weight_grad = call(
        functools.partial(combine_body, cap, pad, experts),
        [struct((rows, depth)), struct((top, rows))],
        "combine",
        flops=2 * experts * pad * rows * depth,
    )(rel, routes_t, *returned)
    return (token_grad, weight_grad.T, down_grad[None])


def solution(mesh):
    placed = (
        P("ep", "tp"),
        P("ep", "tp"),
        P("ep", None),
        P("ep", None),
        P("ep", None, "tp"),
        P("ep", None, "tp"),
        P("ep", "tp", None),
    )
    return jax.shard_map(
        per_device,
        mesh=mesh,
        in_specs=placed,
        out_specs=(P("ep", "tp"), P("ep", None), P("ep", "tp", None)),
        check_vma=False,
    )
```

```python
import functools
import jax
import jax.numpy as jnp
from jax import lax
from jax.experimental import pallas as pl
from jax.experimental.pallas import tpu as pltpu
from jax.sharding import PartitionSpec as P

clamp_limit = 7.0
alpha_gate = 1.702
lanes = 128
sublanes = 8


VMEM = pl.BlockSpec(memory_space=pltpu.VMEM)
SMEM = pl.BlockSpec(memory_space=pltpu.SMEM)
HBM = pl.BlockSpec(memory_space=pltpu.HBM)
f32 = jnp.float32
bf16 = jnp.bfloat16
rows_by_rows = (((1,), (1,)), ((), ()))
cols_by_cols = (((0,), (0,)), ((), ()))


class Plan:
    def __init__(self, experts, shares, rows, top, depth, width):
        self.experts, self.shares, self.rows, self.top = experts, shares, rows, top
        self.depth, self.width = depth, width
        self.chunks = depth // lanes
        cap = rows * top // experts + 1
        self.over = int(cap - 1 >= sublanes and (cap - 1) & (cap - 2) == 0)
        self.main = cap - 1 if self.over else sublanes
        while self.main + self.over < cap:
            self.main *= 2
        assert self.main <= lanes
        self.by_permute = experts <= 8
        self.groups = [[0, 1, 2, 3], [4, 5], [6, 7]] if experts == 8 else [list(range(experts))]
        self.extra_out = -(-(2 * self.chunks * self.over + 1) // sublanes) * sublanes
        self.block_out = 2 * self.chunks * self.main + self.extra_out
        self.extra_back = -(-(self.chunks * self.over + 4) // sublanes) * sublanes
        self.block_back = self.chunks * self.main + self.extra_back

    def slots(self, blocks):
        return blocks * self.main

    def score_rows(self, blocks):
        return -(-self.slots(blocks) // lanes)

    def extra(self, blocks):
        used = blocks * self.over + 2 * self.score_rows(blocks) + 2
        return -(-used // sublanes) * sublanes

    def height(self, blocks):
        return self.slots(blocks) + self.extra(blocks)

    def pairs(self, blocks):
        base, t = blocks * self.over, self.score_rows(blocks)
        return [(base + i, base + t + i) for i in range(t)] + [(base + 2 * t, base + 2 * t + 1)]


def iota(shape, dim):
    return lax.broadcasted_iota(jnp.int32, shape, dim)


def to_row(col):
    shape = (col.shape[0], lanes)
    return jnp.sum(jnp.where(iota(shape, 0) == iota(shape, 1), col, 0.0), axis=0, keepdims=True)


def to_col(row, n, first=0):
    shape = (n, lanes)
    hit = iota(shape, 0) + first == iota(shape, 1)
    return jnp.sum(jnp.where(hit, row, 0.0), axis=1, keepdims=True)


def stack_rows(rows, height):
    at = iota((height, rows[0].shape[1]), 0)
    out = jnp.zeros((height, rows[0].shape[1]), f32)
    for i, row in enumerate(rows):
        out = jnp.where(at == i, row, out)
    return out


def call(body, out, in_hbm=0, scratch=()):
    def run(scalars, *args):
        kernel = pl.pallas_call(
            body,
            out_shape=out,
            in_specs=[SMEM] + [HBM] * in_hbm + [VMEM] * (len(args) - in_hbm),
            out_specs=jax.tree.map(lambda _: VMEM, out),
            scratch_shapes=scratch,
            compiler_params=pltpu.CompilerParams(vmem_limit_bytes=16 << 20),
            cost_estimate=pl.CostEstimate(
                flops=1 << 28, bytes_accessed=1 << 20, transcendentals=0
            ),
        )
        fixed = [pltpu.with_memory_space_constraint(a, pltpu.HBM) for a in args[:in_hbm]]
        return kernel(scalars, *fixed, *args[in_hbm:])

    return run


def names(plan, spot, routes_t):
    me = spot // plan.shares if plan.by_permute else 0
    ids = iota((plan.experts, plan.rows), 0)
    return [ids == (routes_t[k : k + 1, :] ^ me) for k in range(plan.top)]


def load_body(n, s_ref, *refs):
    sources, outs, sems = refs[:n], refs[-n - 1 : -1], refs[-1]
    copies = [pltpu.make_async_copy(sources[i], outs[i], sems.at[i]) for i in range(n)]
    for copy in copies:
        copy.start()
    for copy in copies:
        copy.wait()


def join_body(s_ref, *refs):
    out = refs[-1]
    high = refs[0].shape[0]
    for b, ref in enumerate(refs[:-1]):
        out[b * high : (b + 1) * high, :] = ref[...]


def dispatch_body(plan, s_ref, *refs):
    outs, (pick_ref, over_ref, again_ref) = refs[4:-8], refs[-8:-5]
    held, sems = refs[-5:-1], refs[-1]
    copies = [pltpu.make_async_copy(refs[i], held[i], sems.at[i]) for i in range(4)]
    for copy in copies:
        copy.start()
    routes_ref, weights_ref, tok_ref, cot_ref = held
    copies[0].wait()
    copies[1].wait()
    rows, main, chunks = plan.rows, plan.main, plan.chunks
    again_ref[...] = routes_ref[...]
    named = names(plan, s_ref[0], routes_ref[...])
    any_named = functools.reduce(jnp.logical_or, named)
    before = (iota((rows, rows), 0) < iota((rows, rows), 1)).astype(bf16)
    ranks = jnp.dot(any_named.astype(bf16), before, preferred_element_type=f32)
    place = jnp.where(any_named, ranks, -1.0)
    weights = weights_ref[...].astype(f32)
    scale = functools.reduce(
        jnp.add, [jnp.where(named[k], weights[k : k + 1, :], 0.0) for k in range(plan.top)]
    )
    want = iota((main, rows), 0).astype(f32)
    pick = jnp.concatenate(
        [(place[e : e + 1, :] == want).astype(bf16) for e in range(plan.experts)], axis=0
    )
    pick_over = (place == float(main)).astype(f32)
    pick_ref[...] = pick
    over_ref[...] = pick_over.astype(bf16)
    copies[2].wait()
    copies[3].wait()
    x = jnp.dot(pick, tok_ref[...], preferred_element_type=f32).astype(bf16)
    g = jnp.dot(pick, cot_ref[...], preferred_element_type=f32).astype(bf16)
    if plan.over:
        over_x = jnp.dot(pick_over.astype(bf16), tok_ref[...], preferred_element_type=f32)
        over_g = jnp.dot(pick_over.astype(bf16), cot_ref[...], preferred_element_type=f32)
        over_scale = jnp.sum(pick_over * scale, axis=1, keepdims=True)
    for e in range(plan.experts):
        out = outs[e] if plan.by_permute else outs[0].at[e]
        low, high = e * main, (e + 1) * main
        for half, value in enumerate((x, g)):
            for c in range(chunks):
                at = (half * chunks + c) * main
                out[at : at + main, :] = value[low:high, c * lanes : (c + 1) * lanes]
        col = jnp.sum(
            pick[low:high, :].astype(f32) * scale[e : e + 1, :], axis=1, keepdims=True
        )
        row = to_row(col)
        parts = []
        if plan.over:
            row = jnp.where(iota((1, lanes), 1) == main, over_scale[e : e + 1, :], row)
            for value in (over_x, over_g):
                parts += [
                    value[e : e + 1, c * lanes : (c + 1) * lanes] for c in range(chunks)
                ]
        out[2 * chunks * main :, :] = stack_rows(parts + [row], plan.extra_out).astype(bf16)


def unpack(plan, ref, first):
    main, chunks = plan.main, plan.chunks
    blocks = ref.shape[0] // plan.block_out
    mains, overs = [], []
    for b in range(blocks):
        low = b * plan.block_out
        mains.append(
            jnp.concatenate(
                [
                    ref[low + (first + c) * main : low + (first + c + 1) * main, :]
                    for c in range(chunks)
                ],
                axis=1,
            )
        )
        if plan.over:
            end = low + 2 * chunks * main
            tile = ref[end : end + plan.extra_out, :].astype(f32)
            overs.append(
                jnp.concatenate(
                    [tile[first + c : first + c + 1, :] for c in range(chunks)], axis=1
                )
            )
    extra = plan.extra(blocks)
    if overs:
        tail = stack_rows(overs, extra).astype(bf16)
    else:
        tail = jnp.zeros((extra, plan.depth), bf16)
    return jnp.concatenate(mains + [tail], axis=0)


def scales_of(plan, ref):
    blocks = ref.shape[0] // plan.block_out
    cols, overs = [], []
    for b in range(blocks):
        end = b * plan.block_out + 2 * plan.chunks * plan.main
        tile = ref[end : end + plan.extra_out, :].astype(f32)
        at = 2 * plan.chunks * plan.over
        row = tile[at : at + 1, :]
        cols.append(to_col(row, plan.main))
        overs.append(to_col(row, 1, plan.main) if plan.over else jnp.zeros((1, 1), f32))
    extra = plan.extra(blocks)
    if plan.over:
        cols.append(stack_rows(overs, extra))
    else:
        cols.append(jnp.zeros((extra, 1), f32))
    return jnp.concatenate(cols, axis=0)


def feats(plan, spot, j):
    share = (spot % plan.shares) ^ j
    return pl.ds(pl.multiple_of(share * plan.depth, lanes), plan.depth)


def products(plan, spot, weights, parts, which):
    gate_ref, up_ref, down_ref = weights
    sums = [None, None, None]
    for ref, j in zip(parts, which):
        at = feats(plan, spot, j)
        x, g = unpack(plan, ref, 0), unpack(plan, ref, plan.chunks)
        new = (
            jnp.dot(x, gate_ref[at, :], preferred_element_type=f32),
            jnp.dot(x, up_ref[at, :], preferred_element_type=f32),
            lax.dot_general(g, down_ref[:, at], rows_by_rows, preferred_element_type=f32),
        )
        sums = [n if s is None else s + n for s, n in zip(sums, new)]
    return sums


def part_body(plan, which, s_ref, *refs):
    weights, parts, outs = refs[:3], refs[3:-3], refs[-3:]
    for out, value in zip(outs, products(plan, s_ref[0], weights, parts, which)):
        out[...] = value


def shares_of_rows(plan, spot, weights, grads, scores, which, out):
    gate_ref, up_ref = weights
    gate_grad, up_grad = grads
    slots = out.shape[0] - scores.shape[0]
    base = slots // plan.main * plan.over
    put = iota(scores.shape, 0) >= base
    for i, j in enumerate(which):
        at = feats(plan, spot, j)
        part = lax.dot_general(
            gate_grad, gate_ref[at, :], rows_by_rows, preferred_element_type=f32
        ) + lax.dot_general(up_grad, up_ref[at, :], rows_by_rows, preferred_element_type=f32)
        low = i * plan.depth
        out[:slots, low : low + plan.depth] = part[:slots, :].astype(bf16)
        out[slots:, low + lanes : low + plan.depth] = part[slots:, lanes:].astype(bf16)
        out[slots:, low : low + lanes] = jnp.where(put, scores, part[slots:, :lanes]).astype(bf16)


def split_sums(plan, blocks, tile):
    at = iota(tile.shape, 0)
    out = tile
    for high, low in plan.pairs(blocks):
        row = tile[high : high + 1, :] + tile[low : low + 1, :]
        first = row.astype(bf16).astype(f32)
        out = jnp.where(at == high, first, out)
        out = jnp.where(at == low, row - first, out)
    return out


def grads_body(plan, which, s_ref, *refs):
    weights, sums, own_ref, parts = refs[:3], refs[3:6], refs[6], refs[7:-5]
    send_ref, gate_out, up_out, weighted_ref, score_ref = refs[-5:]
    blocks = own_ref.shape[0] // plan.block_out
    slots = plan.slots(blocks)
    gate_pre, up_pre, back = [
        s[...] + n for s, n in zip(sums, products(plan, s_ref[0], weights, parts, which))
    ]
    gate_clip = jnp.minimum(gate_pre, clamp_limit)
    up_one = jnp.clip(up_pre, -clamp_limit, clamp_limit) + 1.0
    sig = jax.nn.sigmoid(alpha_gate * gate_clip)
    swish = gate_clip * sig
    hidden = up_one * swish
    weight = scales_of(plan, own_ref)
    scaled = back * weight
    slope = sig + alpha_gate * swish * (1.0 - sig)
    gate_grad = jnp.where(gate_pre < clamp_limit, scaled * up_one * slope, 0.0).astype(bf16)
    up_grad = jnp.where(jnp.abs(up_pre) < clamp_limit, scaled * swish, 0.0).astype(bf16)
    gate_out[...] = gate_grad
    up_out[...] = up_grad
    weighted_ref[...] = (hidden * weight).astype(bf16)
    scores = jnp.sum(hidden * back, axis=1, keepdims=True)
    totals = [
        to_row(scores[low : min(low + lanes, slots), :]) for low in range(0, slots, lanes)
    ]
    totals.append(to_row(scores[slots : slots + sublanes, :]))
    blank = [jnp.zeros((1, lanes), f32)]
    n = len(totals) - 1
    rows = blank * (blocks * plan.over) + totals[:n] + blank * n + totals[n:] + blank
    tile = split_sums(plan, blocks, stack_rows(rows, plan.extra(blocks)))
    score_ref[...] = tile
    shares_of_rows(
        plan, s_ref[0], weights[:2], (gate_grad, up_grad), tile, (1, 3), send_ref
    )


def keep_body(plan, s_ref, gate_ref, up_ref, gate_grad, up_grad, score_ref, out):
    shares_of_rows(
        plan,
        s_ref[0],
        (gate_ref, up_ref),
        (gate_grad[...], up_grad[...]),
        score_ref[...],
        (0, 2),
        out,
    )


def add_body(plan, blocks, s_ref, a_ref, b_ref, keep_ref, send_ref):
    tot = a_ref[...].astype(f32) + b_ref[...].astype(f32)
    slots, depth = plan.slots(blocks), plan.depth
    keep_ref[...] = tot[:, :depth]
    send_ref[:slots, :] = tot[:slots, depth:].astype(bf16)
    send_ref[slots:, lanes:] = tot[slots:, depth + lanes :].astype(bf16)
    send_ref[slots:, :lanes] = split_sums(
        plan, blocks, tot[slots:, depth : depth + lanes]
    ).astype(bf16)


def last_body(plan, blocks, s_ref, a_ref, b_ref, *outs):
    tot = a_ref[...] + b_ref[...].astype(f32)
    slots, main, chunks = plan.slots(blocks), plan.main, plan.chunks
    tail = tot[slots:, :]
    sums = split_sums(plan, blocks, tail[:, :lanes])
    pairs = plan.pairs(blocks)
    for b in range(blocks):
        out = outs[b] if plan.by_permute else outs[0].at[b]
        for c in range(chunks):
            out[c * main : (c + 1) * main, :] = tot[
                b * main : (b + 1) * main, c * lanes : (c + 1) * lanes
            ].astype(bf16)
        rows = []
        if plan.over:
            rows = [tail[b : b + 1, c * lanes : (c + 1) * lanes] for c in range(chunks)]
        for high, low in (pairs[b * main // lanes], pairs[-1]):
            rows += [sums[high : high + 1, :], sums[low : low + 1, :]]
        out[chunks * main :, :] = stack_rows(rows, plan.extra_back).astype(bf16)


def down_body(plan, s_ref, *refs):
    out, groups = refs[-1], refs[:-1]
    step = plan.shares + 1
    for j in range(plan.shares):
        acc = None
        for i in range(0, len(groups), step):
            g = unpack(plan, groups[i + 1 + j], plan.chunks)
            part = lax.dot_general(groups[i][...], g, cols_by_cols, preferred_element_type=f32)
            acc = part if acc is None else acc + part
        out[:, feats(plan, s_ref[0], j)] = acc.astype(bf16)


def combine_body(plan, s_ref, routes_ref, pick_ref, over_ref, *refs):
    blocks, (tok_ref, wgt_ref) = refs[:-2], refs[-2:]
    main, chunks = plan.main, plan.chunks
    at_block = {k: b for ks in plan.groups for b, k in enumerate(ks)}
    mine = s_ref[0] // plan.shares
    pick = pick_ref[...]
    pick_over = over_ref[...].astype(f32)
    mains, overs, scores = [], [], []
    for e in range(plan.experts):
        ref = blocks[e] if plan.by_permute else blocks[0].at[e]
        place = at_block[e] if plan.by_permute else mine
        mains.append(
            jnp.concatenate(
                [ref[c * main : (c + 1) * main, :] for c in range(chunks)], axis=1
            )
        )
        tile = ref[chunks * main :, :].astype(f32)
        base = chunks * plan.over
        if plan.over:
            overs.append(
                jnp.concatenate([tile[c : c + 1, :] for c in range(chunks)], axis=1)
            )
        row = tile[base : base + 1, :] + tile[base + 1 : base + 2, :]
        col = to_col(row, main, place * main % lanes)
        hit = pick[e * main : (e + 1) * main, :].astype(f32)
        score = jnp.sum(hit * col, axis=0, keepdims=True)
        if plan.over:
            row = tile[base + 2 : base + 3, :] + tile[base + 3 : base + 4, :]
            score = score + pick_over[e : e + 1, :] * to_col(row, 1, place)
        scores.append(score)
    tot = lax.dot_general(
        pick, jnp.concatenate(mains, axis=0), cols_by_cols, preferred_element_type=f32
    )
    if plan.over:
        tot = tot + lax.dot_general(
            over_ref[...],
            stack_rows(overs, plan.experts).astype(bf16),
            cols_by_cols,
            preferred_element_type=f32,
        )
    tok_ref[...] = tot.astype(bf16)
    scores = jnp.concatenate(scores, axis=0)
    for k, named in enumerate(names(plan, s_ref[0], routes_ref[...])):
        wgt_ref[k : k + 1, :] = jnp.sum(
            jnp.where(named, scores, 0.0), axis=0, keepdims=True
        ).astype(bf16)


def struct(shape, dtype=bf16):
    return jax.ShapeDtypeStruct(shape, dtype)


def per_device(tokens, cotangent, routes, route_weights, gate_weight, up_weight, down_weight):
    experts = lax.axis_size("ep")
    shares = lax.axis_size("tp")
    rows, top = routes.shape
    depth = tokens.shape[1]
    width = gate_weight.shape[2]
    plan = Plan(experts, shares, rows, top, depth, width)
    spot = lax.axis_index("ep") * shares + lax.axis_index("tp")
    spot = spot.astype(jnp.int32).reshape(1)
    gate, up, down = gate_weight[0], up_weight[0], down_weight[0]
    routes_t, weights_t = routes.T, route_weights.T

    def kernel(body, out, **kwargs):
        return functools.partial(call(body, out, **kwargs), spot)

    def over_tp(v, flip):
        return lax.ppermute(v, "tp", [(i, i ^ flip) for i in range(shares)])

    def over_ep(v, flip):
        return lax.ppermute(v, "ep", [(i, i ^ flip) for i in range(experts)])

    def all_over_ep(v):
        return lax.all_to_all(v, "ep", split_axis=0, concat_axis=0, tiled=True)

    def per_block(n, height):
        if plan.by_permute:
            return [struct((height, lanes))] * n
        return [struct((n, height, lanes))]

    *blocks, pick, pick_over, routes_again = kernel(
        functools.partial(dispatch_body, plan),
        per_block(experts, plan.block_out)
        + [
            struct((experts * plan.main, rows)),
            struct((experts, rows)),
            struct((top, rows), jnp.int32),
        ],
        in_hbm=4,
        scratch=[
            pltpu.VMEM((top, rows), jnp.int32),
            pltpu.VMEM((top, rows), bf16),
            pltpu.VMEM((rows, depth), bf16),
            pltpu.VMEM((rows, depth), bf16),
            pltpu.SemaphoreType.DMA((4,)),
        ],
    )(routes_t, weights_t, tokens, cotangent)
    weights = kernel(
        functools.partial(load_body, 3),
        [struct(w.shape) for w in (gate, up, down)],
        in_hbm=3,
        scratch=[pltpu.SemaphoreType.DMA((3,))],
    )(gate, up, down)
    if plan.by_permute:
        moved = [blocks[0]] + [over_ep(blocks[k], k) for k in range(1, experts)]
        groups = [
            kernel(join_body, struct((len(ks) * plan.block_out, lanes)))(*[moved[k] for k in ks])
            for ks in plan.groups
        ]
    else:
        groups = [all_over_ep(blocks[0]).reshape(experts * plan.block_out, lanes)]

    down_args, returned = [], {}
    for g, own in enumerate(groups):
        n = len(plan.groups[g])
        high = plan.height(n)
        across = over_tp(own, 2)
        beside = over_tp(own, 1)
        far = over_tp(across, 1)
        sums = kernel(
            functools.partial(part_body, plan, (0, 1)), [struct((high, width), f32)] * 3
        )(*weights, own, beside)
        send, gate_grad, up_grad, weighted, scores = kernel(
            functools.partial(grads_body, plan, (2, 3)),
            [struct((high, 2 * depth))]
            + [struct((high, width))] * 3
            + [struct((plan.extra(n), lanes), f32)],
        )(*weights, *sums, own, across, far)
        got = over_tp(send, 1)
        keep = kernel(
            functools.partial(keep_body, plan), struct((high, 2 * depth))
        )(*weights[:2], gate_grad, up_grad, scores)
        keep, send = kernel(
            functools.partial(add_body, plan, n),
            [struct((high, depth), f32), struct((high, depth))],
        )(keep, got)
        got = over_tp(send, 2)
        last = kernel(
            functools.partial(last_body, plan, n), per_block(n, plan.block_back)
        )(keep, got)
        returned.update(zip(plan.groups[g], last))
        down_args += [weighted, own, beside, across, far]
    if plan.by_permute:
        back = [returned[0]] + [over_ep(returned[k], k) for k in range(1, experts)]
    else:
        back = [all_over_ep(returned[0])]
    down_grad = kernel(
        functools.partial(down_body, plan), struct((width, shares * depth))
    )(*down_args)
    token_grad, weight_grad = kernel(
        functools.partial(combine_body, plan), [struct((rows, depth)), struct((top, rows))]
    )(routes_again, pick, pick_over, *back)
    return (token_grad, weight_grad.T, down_grad[None])


def solution(mesh):
    placed = (
        P("ep", "tp"),
        P("ep", "tp"),
        P("ep", None),
        P("ep", None),
        P("ep", None, "tp"),
        P("ep", None, "tp"),
        P("ep", "tp", None),
    )

    return jax.shard_map(
        per_device,
        mesh=mesh,
        in_specs=placed,
        out_specs=(P("ep", "tp"), P("ep", None), P("ep", "tp", None)),
        check_vma=False,
    )
```

```python
import functools
import jax
import jax.numpy as jnp
from jax import lax
from jax.experimental import pallas as pl
from jax.experimental.pallas import tpu as pltpu
from jax.sharding import PartitionSpec as P

clamp_limit = 7.0
alpha_gate = 1.702
lanes = 128
sublanes = 8


VMEM = pl.BlockSpec(memory_space=pltpu.VMEM)
SMEM = pl.BlockSpec(memory_space=pltpu.SMEM)
HBM = pl.BlockSpec(memory_space=pltpu.HBM)
f32 = jnp.float32
bf16 = jnp.bfloat16
rows_by_rows = (((1,), (1,)), ((), ()))
cols_by_cols = (((0,), (0,)), ((), ()))


class Plan:
    def __init__(self, experts, shares, rows, top, depth, width):
        self.experts, self.shares, self.rows, self.top = experts, shares, rows, top
        self.depth, self.width = depth, width
        self.chunks = depth // lanes
        cap = rows * top // experts + 1
        self.over = int(cap - 1 >= sublanes and (cap - 1) & (cap - 2) == 0)
        self.main = cap - 1 if self.over else sublanes
        while self.main + self.over < cap:
            self.main *= 2
        assert self.main <= lanes
        self.by_permute = experts == 8
        self.groups = [[0, 1, 2, 3], [4, 5], [6, 7]] if self.by_permute else [list(range(experts))]
        self.home = [(0, 0), (4, 0), (1, 0), (4, 1), (2, 0), (4, 2), (3, 0), (5, 0)]
        self.extra_out = -(-(2 * self.chunks * self.over + 1) // sublanes) * sublanes
        self.block_out = 2 * self.chunks * self.main + self.extra_out
        self.extra_back = -(-(self.chunks * self.over + 4) // sublanes) * sublanes
        self.block_back = self.chunks * self.main + self.extra_back

    def slots(self, blocks):
        return blocks * self.main

    def score_rows(self, blocks):
        return -(-self.slots(blocks) // lanes)

    def extra(self, blocks):
        used = blocks * self.over + 2 * self.score_rows(blocks) + 2
        return -(-used // sublanes) * sublanes

    def height(self, blocks):
        return self.slots(blocks) + self.extra(blocks)

    def pairs(self, blocks):
        base, t = blocks * self.over, self.score_rows(blocks)
        return [(base + i, base + t + i) for i in range(t)] + [(base + 2 * t, base + 2 * t + 1)]


def iota(shape, dim):
    return lax.broadcasted_iota(jnp.int32, shape, dim)


def to_row(col):
    shape = (col.shape[0], lanes)
    return jnp.sum(jnp.where(iota(shape, 0) == iota(shape, 1), col, 0.0), axis=0, keepdims=True)


def to_col(row, n, first=0):
    shape = (n, lanes)
    hit = iota(shape, 0) + first == iota(shape, 1)
    return jnp.sum(jnp.where(hit, row, 0.0), axis=1, keepdims=True)


def stack_rows(rows, height):
    at = iota((height, rows[0].shape[1]), 0)
    out = jnp.zeros((height, rows[0].shape[1]), f32)
    for i, row in enumerate(rows):
        out = jnp.where(at == i, row, out)
    return out


def call(body, out, in_hbm=0, scratch=()):
    def run(scalars, *args):
        kernel = pl.pallas_call(
            body,
            out_shape=out,
            in_specs=[SMEM] + [HBM] * in_hbm + [VMEM] * (len(args) - in_hbm),
            out_specs=jax.tree.map(lambda _: VMEM, out),
            scratch_shapes=scratch,
            compiler_params=pltpu.CompilerParams(vmem_limit_bytes=16 << 20),
            cost_estimate=pl.CostEstimate(
                flops=1 << 28, bytes_accessed=1 << 20, transcendentals=0
            ),
        )
        fixed = [pltpu.with_memory_space_constraint(a, pltpu.HBM) for a in args[:in_hbm]]
        return kernel(scalars, *fixed, *args[in_hbm:])

    return run


def names(plan, spot, routes_t):
    me = spot // plan.shares if plan.by_permute else 0
    ids = iota((plan.experts, plan.rows), 0)
    return [ids == (routes_t[k : k + 1, :] ^ me) for k in range(plan.top)]


def load_body(n, s_ref, *refs):
    sources, outs, sems = refs[:n], refs[-n - 1 : -1], refs[-1]
    copies = [pltpu.make_async_copy(sources[i], outs[i], sems.at[i]) for i in range(n)]
    for copy in copies:
        copy.start()
    for copy in copies:
        copy.wait()


def join_body(s_ref, *refs):
    out = refs[-1]
    high = refs[0].shape[0]
    for b, ref in enumerate(refs[:-1]):
        out[b * high : (b + 1) * high, :] = ref[...]


def dispatch_body(plan, s_ref, *refs):
    outs, (pick_ref, over_ref, again_ref) = refs[4:-8], refs[-8:-5]
    held, sems = refs[-5:-1], refs[-1]
    copies = [pltpu.make_async_copy(refs[i], held[i], sems.at[i]) for i in range(4)]
    for copy in copies:
        copy.start()
    routes_ref, weights_ref, tok_ref, cot_ref = held
    copies[0].wait()
    copies[1].wait()
    rows, main, chunks = plan.rows, plan.main, plan.chunks
    again_ref[...] = routes_ref[...]
    named = names(plan, s_ref[0], routes_ref[...])
    any_named = functools.reduce(jnp.logical_or, named)
    before = (iota((rows, rows), 0) < iota((rows, rows), 1)).astype(bf16)
    ranks = jnp.dot(any_named.astype(bf16), before, preferred_element_type=f32)
    place = jnp.where(any_named, ranks, -1.0)
    weights = weights_ref[...].astype(f32)
    scale = functools.reduce(
        jnp.add, [jnp.where(named[k], weights[k : k + 1, :], 0.0) for k in range(plan.top)]
    )
    want = iota((main, rows), 0).astype(f32)
    pick = jnp.concatenate(
        [(place[e : e + 1, :] == want).astype(bf16) for e in range(plan.experts)], axis=0
    )
    pick_over = (place == float(main)).astype(f32)
    pick_ref[...] = pick
    over_ref[...] = pick_over.astype(bf16)
    copies[2].wait()
    copies[3].wait()
    x = jnp.dot(pick, tok_ref[...], preferred_element_type=f32).astype(bf16)
    g = jnp.dot(pick, cot_ref[...], preferred_element_type=f32).astype(bf16)
    if plan.over:
        over_x = jnp.dot(pick_over.astype(bf16), tok_ref[...], preferred_element_type=f32)
        over_g = jnp.dot(pick_over.astype(bf16), cot_ref[...], preferred_element_type=f32)
        over_scale = jnp.sum(pick_over * scale, axis=1, keepdims=True)
    for e in range(plan.experts):
        out = outs[e] if plan.by_permute else outs[0].at[e]
        low, high = e * main, (e + 1) * main
        for half, value in enumerate((x, g)):
            for c in range(chunks):
                at = (half * chunks + c) * main
                out[at : at + main, :] = value[low:high, c * lanes : (c + 1) * lanes]
        col = jnp.sum(
            pick[low:high, :].astype(f32) * scale[e : e + 1, :], axis=1, keepdims=True
        )
        row = to_row(col)
        parts = []
        if plan.over:
            row = jnp.where(iota((1, lanes), 1) == main, over_scale[e : e + 1, :], row)
            for value in (over_x, over_g):
                parts += [
                    value[e : e + 1, c * lanes : (c + 1) * lanes] for c in range(chunks)
                ]
        out[2 * chunks * main :, :] = stack_rows(parts + [row], plan.extra_out).astype(bf16)


def unpack(plan, ref, first):
    main, chunks = plan.main, plan.chunks
    blocks = ref.shape[0] // plan.block_out
    mains, overs = [], []
    for b in range(blocks):
        low = b * plan.block_out
        mains.append(
            jnp.concatenate(
                [
                    ref[low + (first + c) * main : low + (first + c + 1) * main, :]
                    for c in range(chunks)
                ],
                axis=1,
            )
        )
        if plan.over:
            end = low + 2 * chunks * main
            tile = ref[end : end + plan.extra_out, :].astype(f32)
            overs.append(
                jnp.concatenate(
                    [tile[first + c : first + c + 1, :] for c in range(chunks)], axis=1
                )
            )
    extra = plan.extra(blocks)
    if overs:
        tail = stack_rows(overs, extra).astype(bf16)
    else:
        tail = jnp.zeros((extra, plan.depth), bf16)
    return jnp.concatenate(mains + [tail], axis=0)


def scales_of(plan, ref):
    blocks = ref.shape[0] // plan.block_out
    cols, overs = [], []
    for b in range(blocks):
        end = b * plan.block_out + 2 * plan.chunks * plan.main
        tile = ref[end : end + plan.extra_out, :].astype(f32)
        at = 2 * plan.chunks * plan.over
        row = tile[at : at + 1, :]
        cols.append(to_col(row, plan.main))
        overs.append(to_col(row, 1, plan.main) if plan.over else jnp.zeros((1, 1), f32))
    extra = plan.extra(blocks)
    if plan.over:
        cols.append(stack_rows(overs, extra))
    else:
        cols.append(jnp.zeros((extra, 1), f32))
    return jnp.concatenate(cols, axis=0)


def feats(plan, spot, j):
    share = (spot % plan.shares) ^ j
    return pl.ds(pl.multiple_of(share * plan.depth, lanes), plan.depth)


def products(plan, spot, weights, parts, which):
    gate_ref, up_ref, down_ref = weights
    sums = [None, None, None]
    for ref, j in zip(parts, which):
        at = feats(plan, spot, j)
        x, g = unpack(plan, ref, 0), unpack(plan, ref, plan.chunks)
        new = (
            jnp.dot(x, gate_ref[at, :], preferred_element_type=f32),
            jnp.dot(x, up_ref[at, :], preferred_element_type=f32),
            lax.dot_general(g, down_ref[:, at], rows_by_rows, preferred_element_type=f32),
        )
        sums = [n if s is None else s + n for s, n in zip(sums, new)]
    return sums


def part_body(plan, which, s_ref, *refs):
    weights, parts, outs = refs[:3], refs[3:-3], refs[-3:]
    for out, value in zip(outs, products(plan, s_ref[0], weights, parts, which)):
        out[...] = value


def shares_of_rows(plan, spot, weights, grads, scores, which, out):
    gate_ref, up_ref = weights
    gate_grad, up_grad = grads
    slots = out.shape[0] - scores.shape[0]
    base = slots // plan.main * plan.over
    put = iota(scores.shape, 0) >= base
    for i, j in enumerate(which):
        at = feats(plan, spot, j)
        part = lax.dot_general(
            gate_grad, gate_ref[at, :], rows_by_rows, preferred_element_type=f32
        ) + lax.dot_general(up_grad, up_ref[at, :], rows_by_rows, preferred_element_type=f32)
        low = i * plan.depth
        out[:slots, low : low + plan.depth] = part[:slots, :].astype(bf16)
        out[slots:, low + lanes : low + plan.depth] = part[slots:, lanes:].astype(bf16)
        out[slots:, low : low + lanes] = jnp.where(put, scores, part[slots:, :lanes]).astype(bf16)


def split_sums(plan, blocks, tile):
    at = iota(tile.shape, 0)
    out = tile
    for high, low in plan.pairs(blocks):
        row = tile[high : high + 1, :] + tile[low : low + 1, :]
        first = row.astype(bf16).astype(f32)
        out = jnp.where(at == high, first, out)
        out = jnp.where(at == low, row - first, out)
    return out


def grads_body(plan, which, s_ref, *refs):
    weights, sums, own_ref, parts = refs[:3], refs[3:6], refs[6], refs[7:-5]
    send_ref, gate_out, up_out, weighted_ref, score_ref = refs[-5:]
    blocks = own_ref.shape[0] // plan.block_out
    slots = plan.slots(blocks)
    gate_pre, up_pre, back = [
        s[...] + n for s, n in zip(sums, products(plan, s_ref[0], weights, parts, which))
    ]
    gate_clip = jnp.minimum(gate_pre, clamp_limit)
    up_one = jnp.clip(up_pre, -clamp_limit, clamp_limit) + 1.0
    sig = jax.nn.sigmoid(alpha_gate * gate_clip)
    swish = gate_clip * sig
    hidden = up_one * swish
    weight = scales_of(plan, own_ref)
    scaled = back * weight
    slope = sig + alpha_gate * swish * (1.0 - sig)
    gate_grad = jnp.where(gate_pre < clamp_limit, scaled * up_one * slope, 0.0).astype(bf16)
    up_grad = jnp.where(jnp.abs(up_pre) < clamp_limit, scaled * swish, 0.0).astype(bf16)
    gate_out[...] = gate_grad
    up_out[...] = up_grad
    weighted_ref[...] = (hidden * weight).astype(bf16)
    scores = jnp.sum(hidden * back, axis=1, keepdims=True)
    totals = [
        to_row(scores[low : min(low + lanes, slots), :]) for low in range(0, slots, lanes)
    ]
    totals.append(to_row(scores[slots : slots + sublanes, :]))
    blank = [jnp.zeros((1, lanes), f32)]
    n = len(totals) - 1
    rows = blank * (blocks * plan.over) + totals[:n] + blank * n + totals[n:] + blank
    tile = split_sums(plan, blocks, stack_rows(rows, plan.extra(blocks)))
    score_ref[...] = tile
    shares_of_rows(
        plan, s_ref[0], weights[:2], (gate_grad, up_grad), tile, (1, 3), send_ref
    )


def keep_body(plan, s_ref, gate_ref, up_ref, gate_grad, up_grad, score_ref, out):
    shares_of_rows(
        plan,
        s_ref[0],
        (gate_ref, up_ref),
        (gate_grad[...], up_grad[...]),
        score_ref[...],
        (0, 2),
        out,
    )


def add_body(plan, blocks, s_ref, a_ref, b_ref, keep_ref, send_ref):
    tot = a_ref[...].astype(f32) + b_ref[...].astype(f32)
    slots, depth = plan.slots(blocks), plan.depth
    keep_ref[...] = tot[:, :depth]
    send_ref[:slots, :] = tot[:slots, depth:].astype(bf16)
    send_ref[slots:, lanes:] = tot[slots:, depth + lanes :].astype(bf16)
    send_ref[slots:, :lanes] = split_sums(
        plan, blocks, tot[slots:, depth : depth + lanes]
    ).astype(bf16)


def block_of(plan, refs, b):
    if not plan.by_permute:
        return refs[0].at[b]
    for ref in refs:
        n = ref.shape[0] // plan.block_back
        if b < n:
            return ref.at[b * plan.block_back : (b + 1) * plan.block_back, :]
        b -= n


def pack_body(plan, picks, s_ref, *refs):
    out, high = refs[-1], plan.block_back
    for i, (r, b) in enumerate(picks):
        out[i * high : (i + 1) * high, :] = refs[r][b * high : (b + 1) * high, :]


def last_body(plan, blocks, s_ref, a_ref, b_ref, *outs):
    tot = a_ref[...] + b_ref[...].astype(f32)
    slots, main, chunks = plan.slots(blocks), plan.main, plan.chunks
    tail = tot[slots:, :]
    sums = split_sums(plan, blocks, tail[:, :lanes])
    pairs = plan.pairs(blocks)
    for b in range(blocks):
        out = block_of(plan, outs, b)
        for c in range(chunks):
            out[c * main : (c + 1) * main, :] = tot[
                b * main : (b + 1) * main, c * lanes : (c + 1) * lanes
            ].astype(bf16)
        rows = []
        if plan.over:
            rows = [tail[b : b + 1, c * lanes : (c + 1) * lanes] for c in range(chunks)]
        for high, low in (pairs[b * main // lanes], pairs[-1]):
            rows += [sums[high : high + 1, :], sums[low : low + 1, :]]
        out[chunks * main :, :] = stack_rows(rows, plan.extra_back).astype(bf16)


def down_body(plan, s_ref, *refs):
    out, groups = refs[-1], refs[:-1]
    step = plan.shares + 1
    for j in range(plan.shares):
        acc = None
        for i in range(0, len(groups), step):
            g = unpack(plan, groups[i + 1 + j], plan.chunks)
            part = lax.dot_general(groups[i][...], g, cols_by_cols, preferred_element_type=f32)
            acc = part if acc is None else acc + part
        out[:, feats(plan, s_ref[0], j)] = acc.astype(bf16)


def combine_body(plan, s_ref, routes_ref, pick_ref, over_ref, *refs):
    blocks, (tok_ref, wgt_ref) = refs[:-2], refs[-2:]
    main, chunks = plan.main, plan.chunks
    at_block = {k: b for ks in plan.groups for b, k in enumerate(ks)}
    mine = s_ref[0] // plan.shares
    pick = pick_ref[...]
    pick_over = over_ref[...].astype(f32)
    mains, overs, scores = [], [], []
    for e in range(plan.experts):
        if plan.by_permute:
            held, b = plan.home[e]
            ref = blocks[held].at[b * plan.block_back : (b + 1) * plan.block_back, :]
        else:
            ref = blocks[0].at[e]
        place = at_block[e] if plan.by_permute else mine
        mains.append(
            jnp.concatenate(
                [ref[c * main : (c + 1) * main, :] for c in range(chunks)], axis=1
            )
        )
        tile = ref[chunks * main :, :].astype(f32)
        base = chunks * plan.over
        if plan.over:
            overs.append(
                jnp.concatenate([tile[c : c + 1, :] for c in range(chunks)], axis=1)
            )
        row = tile[base : base + 1, :] + tile[base + 1 : base + 2, :]
        col = to_col(row, main, place * main % lanes)
        hit = pick[e * main : (e + 1) * main, :].astype(f32)
        score = jnp.sum(hit * col, axis=0, keepdims=True)
        if plan.over:
            row = tile[base + 2 : base + 3, :] + tile[base + 3 : base + 4, :]
            score = score + pick_over[e : e + 1, :] * to_col(row, 1, place)
        scores.append(score)
    tot = lax.dot_general(
        pick, jnp.concatenate(mains, axis=0), cols_by_cols, preferred_element_type=f32
    )
    if plan.over:
        tot = tot + lax.dot_general(
            over_ref[...],
            stack_rows(overs, plan.experts).astype(bf16),
            cols_by_cols,
            preferred_element_type=f32,
        )
    tok_ref[...] = tot.astype(bf16)
    scores = jnp.concatenate(scores, axis=0)
    for k, named in enumerate(names(plan, s_ref[0], routes_ref[...])):
        wgt_ref[k : k + 1, :] = jnp.sum(
            jnp.where(named, scores, 0.0), axis=0, keepdims=True
        ).astype(bf16)


def struct(shape, dtype=bf16):
    return jax.ShapeDtypeStruct(shape, dtype)


def per_device(tokens, cotangent, routes, route_weights, gate_weight, up_weight, down_weight):
    experts = lax.axis_size("ep")
    shares = lax.axis_size("tp")
    rows, top = routes.shape
    depth = tokens.shape[1]
    width = gate_weight.shape[2]
    plan = Plan(experts, shares, rows, top, depth, width)
    spot = lax.axis_index("ep") * shares + lax.axis_index("tp")
    spot = spot.astype(jnp.int32).reshape(1)
    gate, up, down = gate_weight[0], up_weight[0], down_weight[0]
    routes_t, weights_t = routes.T, route_weights.T

    def kernel(body, out, **kwargs):
        return functools.partial(call(body, out, **kwargs), spot)

    def over_tp(v, flip):
        return lax.ppermute(v, "tp", [(i, i ^ flip) for i in range(shares)])

    def over_ep(v, flip):
        return lax.ppermute(v, "ep", [(i, i ^ flip) for i in range(experts)])

    def all_over_ep(v):
        return lax.all_to_all(v, "ep", split_axis=0, concat_axis=0, tiled=True)

    def per_block(n, height):
        if plan.by_permute:
            return [struct((height, lanes))] * n
        return [struct((n, height, lanes))]

    *blocks, pick, pick_over, routes_again = kernel(
        functools.partial(dispatch_body, plan),
        per_block(experts, plan.block_out)
        + [
            struct((experts * plan.main, rows)),
            struct((experts, rows)),
            struct((top, rows), jnp.int32),
        ],
        in_hbm=4,
        scratch=[
            pltpu.VMEM((top, rows), jnp.int32),
            pltpu.VMEM((top, rows), bf16),
            pltpu.VMEM((rows, depth), bf16),
            pltpu.VMEM((rows, depth), bf16),
            pltpu.SemaphoreType.DMA((4,)),
        ],
    )(routes_t, weights_t, tokens, cotangent)
    weights = kernel(
        functools.partial(load_body, 3),
        [struct(w.shape) for w in (gate, up, down)],
        in_hbm=3,
        scratch=[pltpu.SemaphoreType.DMA((3,))],
    )(gate, up, down)
    if plan.by_permute:
        moved = [blocks[0]] + [over_ep(blocks[k], k) for k in range(1, experts)]
        groups = [
            kernel(join_body, struct((len(ks) * plan.block_out, lanes)))(*[moved[k] for k in ks])
            for ks in plan.groups
        ]
    else:
        groups = [all_over_ep(blocks[0]).reshape(experts * plan.block_out, lanes)]

    down_args, returned = [], {}
    for g, own in enumerate(groups):
        n = len(plan.groups[g])
        high = plan.height(n)
        across = over_tp(own, 2)
        beside = over_tp(own, 1)
        far = over_tp(across, 1)
        sums = kernel(
            functools.partial(part_body, plan, (0, 1)), [struct((high, width), f32)] * 3
        )(*weights, own, beside)
        send, gate_grad, up_grad, weighted, scores = kernel(
            functools.partial(grads_body, plan, (2, 3)),
            [struct((high, 2 * depth))]
            + [struct((high, width))] * 3
            + [struct((plan.extra(n), lanes), f32)],
        )(*weights, *sums, own, across, far)
        got = over_tp(send, 1)
        keep = kernel(
            functools.partial(keep_body, plan), struct((high, 2 * depth))
        )(*weights[:2], gate_grad, up_grad, scores)
        keep, send = kernel(
            functools.partial(add_body, plan, n),
            [struct((high, depth), f32), struct((high, depth))],
        )(keep, got)
        got = over_tp(send, 2)
        if plan.by_permute:
            runs = [[0], [1], [2, 3]] if g == 0 else [plan.groups[g]]
            out = [struct((len(ks) * plan.block_back, lanes)) for ks in runs]
        else:
            runs, out = [[0]], [struct((n, plan.block_back, lanes))]
        last = kernel(functools.partial(last_body, plan, n), out)(keep, got)
        returned.update((ks[0], v) for ks, v in zip(runs, last))
        down_args += [weighted, own, beside, across, far]
    if plan.by_permute:
        near, far, last = [over_ep(returned[k], k) for k in (2, 4, 6)]
        beside = kernel(
            functools.partial(pack_body, plan, ((0, 0), (1, 1), (2, 1))),
            struct((3 * plan.block_back, lanes)),
        )(returned[1], near, far)
        final = kernel(
            functools.partial(pack_body, plan, ((0, 1),)), struct((plan.block_back, lanes))
        )(last)
        back = [returned[0], near, far, last, over_ep(beside, 1), over_ep(final, 1)]
    else:
        back = [all_over_ep(returned[0])]
    down_grad = kernel(
        functools.partial(down_body, plan), struct((width, shares * depth))
    )(*down_args)
    token_grad, weight_grad = kernel(
        functools.partial(combine_body, plan), [struct((rows, depth)), struct((top, rows))]
    )(routes_again, pick, pick_over, *back)
    return (token_grad, weight_grad.T, down_grad[None])


def solution(mesh):
    placed = (
        P("ep", "tp"),
        P("ep", "tp"),
        P("ep", None),
        P("ep", None),
        P("ep", None, "tp"),
        P("ep", None, "tp"),
        P("ep", "tp", None),
    )

    return jax.shard_map(
        per_device,
        mesh=mesh,
        in_specs=placed,
        out_specs=(P("ep", "tp"), P("ep", None), P("ep", "tp", None)),
        check_vma=False,
    )
```
